32 devices in a mesh: ra: 4 (over z), cb: 4 (over y, x), dp: 2 (over core).
Axes of the slice: x: 2, y: 2, z: 4, core: 2. Of those that a mesh axis runs over, the one named last changes fastest.
Arguments:
- carried: bfloat16 [3072, 4096], P('dp', 'ra'), may hold values from -100 to 100
- branch_in: bfloat16 [3072, 4096], P('dp', 'ra'), may hold values from -12 to 12
- gain_in: float32 [4096], P('ra'), may hold values from 0.1 to 1.9
- bias_in: float32 [4096], P('ra'), may hold values from -1.8 to 1.8
- up_weight: bfloat16 [4096, 16384], P('ra', 'cb'), may hold values from -0.125 to 0.125
- down_weight: bfloat16 [16384, 4096], P('cb', 'ra'), may hold values from -0.046875 to 0.046875
- gain_out: float32 [4096], P('ra'), may hold values from 0.1 to 1.9
- bias_out: float32 [4096], P('ra'), may hold values from -1.8 to 1.8
Outputs:
- layer_out: bfloat16 [3072, 4096], P('dp', 'ra')
The draws below stay inside these ranges and needn't reach their ends.
All inputs are finite; a program needn't handle non-finite values.
Results may differ from the reference program's by a relative error of at most 0.006.
Values may be sent and summed in bfloat16 or wider, within the bound.
A program may use at most 128 MiB of HBM per device.

```python
import math
import jax
import jax.numpy as jnp
from jax import lax

D = 4096
FF = 16384
TOKENS = 3072


def draw_carried(key, part):
    keys = jax.random.split(jax.random.fold_in(key, 11), 3)
    columns = jnp.arange(D, dtype=jnp.float32) / D
    column_scale = 0.5 * 3.0 ** columns * jnp.exp(jax.random.uniform(keys[1], (D,), jnp.float32, -0.5, 0.5))
    values = jnp.clip(jax.random.normal(keys[0], (TOKENS, D), jnp.float32), -4.0, 4.0)
    row_scale = jnp.exp(jax.random.uniform(keys[2], (TOKENS, 1), jnp.float32, 0.0, math.log(10.0)))
    return (values * row_scale * column_scale[None, :]).astype(jnp.bfloat16)


def raised(entries, key, source, target, blocks, factor):
    owner, partner = [(jnp.arange(entries.shape[axis_at]) // (entries.shape[axis_at] // blocks)).reshape([-1 if axis == axis_at else 1 for axis in range(entries.ndim)]) for axis_at in (source, target)]
    chosen = jax.random.permutation(key, blocks)[partner]
    strong = (owner == chosen) | (owner == (partner + blocks // 2) % blocks)
    return jnp.where(strong, factor * entries, entries)


def level_of(stream_key, extent, cuts, least, high):
    level = 1.0
    for position, parts in cuts:
        steps = jax.random.uniform(jax.random.fold_in(jax.random.fold_in(stream_key, 6), position), (parts,), jnp.float32, least / len(cuts), high / len(cuts))
        level = level * jnp.repeat(jnp.exp(steps), extent[position] // parts).reshape((-1,) + (1,) * (len(extent) - 1 - position))
    return level


def noise(stream_key, shape, deviation, limit, cuts=(), held_as=jnp.bfloat16):
    drawn = deviation * jax.random.normal(stream_key, shape, jnp.float32)
    if cuts:
        drawn = drawn * level_of(stream_key, shape, cuts, -0.22, 0.18)
    return jnp.clip(drawn, -limit, limit).astype(held_as)


def heavy_noise(rng, extent, scale, reach, shards, heavy, held_as=jnp.bfloat16):
    array = scale * jax.random.normal(rng, extent, jnp.float32)
    if shards:
        array = array * level_of(rng, extent, shards, -0.22, 0.18)
    return jnp.clip(raised(array, jax.random.fold_in(rng, 3), *heavy), -reach, reach).astype(held_as)


def setup_inputs(seed: int = 0) -> dict:
    seeds = jax.random.split(jax.random.key(seed), 9)
    return {
        "carried": draw_carried(jax.random.fold_in(seeds[8], 71), 0),
        "branch_in": noise(seeds[1], (TOKENS, D), 2.0, 12.0, ((0, 2), (1, 4))),
        "gain_in": jnp.clip(1.0 + 0.18 * jax.random.normal(seeds[2], (D,), jnp.float32), 0.1, 1.9),
        "bias_in": noise(seeds[3], (D,), 0.3, 1.8, ((0, 4),), jnp.float32),
        "up_weight": heavy_noise(seeds[4], (D, FF), D ** -0.5, 0.125, ((0, 4), (1, 4)), (0, 1, 4, 2.0)),
        "down_weight": noise(seeds[5], (FF, D), FF ** -0.5, 0.046875, ((0, 4), (1, 4))),
        "gain_out": jnp.clip(1.0 + 0.18 * jax.random.normal(seeds[6], (D,), jnp.float32), 0.1, 1.9),
        "bias_out": noise(seeds[7], (D,), 0.3, 1.8, ((0, 4),), jnp.float32),
    }


residual_scale = 2.0 ** 0.25
norm_eps = 1e-05

def layer_norm(mixed, gain, bias):
    mean = lax.optimization_barrier(jnp.mean(mixed, axis=-1, keepdims=True))
    spread = lax.optimization_barrier(jnp.mean(mixed * mixed, axis=-1, keepdims=True)) - mean * mean
    return (mixed - mean) * jax.lax.rsqrt(spread + norm_eps) * gain + bias

def reference(carried, branch_in, gain_in, bias_in, up_weight, down_weight, gain_out, bias_out):
    mixed_in = residual_scale * carried.astype(jnp.float32) + branch_in.astype(jnp.float32)
    normed = layer_norm(mixed_in, gain_in, bias_in).astype(jnp.bfloat16)
    pre = jnp.dot(normed, up_weight, preferred_element_type=jnp.float32)
    hidden = jnp.square(jnp.maximum(pre, 0.0)).astype(jnp.bfloat16)
    branch_out = jnp.dot(hidden, down_weight, preferred_element_type=jnp.float32)
    mixed_out = residual_scale * normed.astype(jnp.float32) + branch_out
    return layer_norm(mixed_out, gain_out, bias_out).astype(jnp.bfloat16)
```

```python
import functools
import math

import jax
import jax.numpy as jnp
from jax import lax
from jax.experimental import pallas as pl
from jax.experimental.pallas import tpu as pltpu
from jax.sharding import PartitionSpec as P

residual_scale = 2.0**0.25
norm_eps = 1e-05
lookahead = 2


def kernel(n, m, nd, block, x_hbm, w1_hbm, w2_hbm, gain_ref, bias_ref, o_hbm,
           xall, w1s, h, w2, part, rs_src, rs_recv, mixed, st_src, st_recv, fin,
           loc_sem, w1_send, w1_recv, dp_send, dp_recv, xz_r, xz_l, xz_recv,
           xy_send, xy_recv, h_r, h_l, h_recv, rs_send, rs_rcv, st_send, st_rcv,
           fin_send, fin_rcv):
    me, cb, dp = lax.axis_index("ra"), lax.axis_index("cb"), lax.axis_index("dp")
    _, tokens, dl = xall.shape
    fs = w1s.shape[2]
    blocks = tokens // block
    quarter = tokens // m
    rows = block // m
    half = dl // nd
    width = n * dl
    tile = math.gcd(256, math.gcd(fs, dl))

    barrier = pltpu.get_barrier_semaphore()
    for o in range(1, n):
        pl.semaphore_signal(barrier, inc=1, device_id={"ra": lax.rem(me + o, n)})
    for o in range(1, m):
        pl.semaphore_signal(barrier, inc=1, device_id={"cb": lax.rem(cb + o, m)})
    for o in range(1, nd):
        pl.semaphore_signal(barrier, inc=1, device_id={"dp": lax.rem(dp + o, nd)})

    own_x = pltpu.make_async_copy(x_hbm, xall.at[me], loc_sem.at[0])
    own_w1 = pltpu.make_async_copy(
        w1_hbm.at[:, pl.ds(pl.multiple_of(me * fs, fs), fs)], w1s.at[me], loc_sem.at[1])
    own_w2 = pltpu.make_async_copy(w2_hbm, w2, loc_sem.at[2])
    own_x.start()
    own_w1.start()
    own_w2.start()
    pl.semaphore_wait(barrier, n + m + nd - 3)
    own_x.wait()

    def at_rows(start, size):
        return pl.ds(pl.multiple_of(start, size), size)

    def line(ref_of, right_sem, left_sem, recv_sem, src, to_right):
        ref = ref_of(src)
        return pltpu.make_async_remote_copy(
            src_ref=ref, dst_ref=ref,
            send_sem=(right_sem if to_right else left_sem)(src),
            recv_sem=recv_sem(src),
            device_id={"ra": jnp.minimum(me + 1, n - 1) if to_right else jnp.maximum(me - 1, 0)})

    def start_own(make):
        @pl.when(me + 1 < n)
        def _():
            make(me, True).start()

        @pl.when(me >= 1)
        def _():
            make(me, False).start()

    def relay(make, landed):
        for s in range(1, n):
            @pl.when(me - s >= 0)
            def _():
                make(me - s, True).wait_recv()

                @pl.when(me + 1 < n)
                def _():
                    make(me - s, True).start()
                landed(me - s)

            @pl.when(me + s < n)
            def _():
                make(me + s, False).wait_recv()

                @pl.when(me >= 1)
                def _():
                    make(me + s, False).start()
                landed(me + s)

    def line_sent(make):
        for s in range(n):
            @pl.when((me - s >= 0) & (me + 1 < n))
            def _():
                make(me - s, True).wait_send()

            @pl.when((me + s < n) & (me >= 1))
            def _():
                make(me + s, False).wait_send()

    make_x = functools.partial(
        line, lambda s: xall.at[s, at_rows(cb * quarter, quarter)],
        lambda s: xz_r.at[s], lambda s: xz_l.at[s], lambda s: xz_recv.at[s])

    def xy_copy(src, o):
        ref = xall.at[src, at_rows(cb * quarter, quarter)]
        return pltpu.make_async_remote_copy(
            src_ref=ref, dst_ref=ref, send_sem=xy_send.at[src, o], recv_sem=xy_recv.at[src, cb],
            device_id={"cb": lax.rem(cb + o, m)})

    def xy_landed(src, o):
        sender = lax.rem(cb + o, m)
        ref = xall.at[src, at_rows(sender * quarter, quarter)]
        return pltpu.make_async_remote_copy(
            src_ref=ref, dst_ref=ref, send_sem=xy_send.at[src, o], recv_sem=xy_recv.at[src, sender],
            device_id={"cb": sender})

    def w1_copy(o):
        to = lax.rem(me + o, n)
        return pltpu.make_async_remote_copy(
            src_ref=w1_hbm.at[at_rows(dp * half, half), pl.ds(pl.multiple_of(to * fs, fs), fs)],
            dst_ref=w1s.at[me, at_rows(dp * half, half)],
            send_sem=w1_send.at[to], recv_sem=w1_recv.at[me], device_id={"ra": to})

    def w1_landed(o):
        src = lax.rem(me + o, n)
        ref = w1s.at[src, at_rows(dp * half, half)]
        return pltpu.make_async_remote_copy(
            src_ref=ref, dst_ref=ref, send_sem=w1_send.at[src], recv_sem=w1_recv.at[src],
            device_id={"ra": src})

    def dp_copy(o, p):
        src = lax.rem(me + o, n)
        ref = w1s.at[src, at_rows(dp * half, half)]
        return pltpu.make_async_remote_copy(
            src_ref=ref, dst_ref=ref, send_sem=dp_send.at[src, p], recv_sem=dp_recv.at[src, dp],
            device_id={"dp": lax.rem(dp + p, nd)})

    def dp_landed(o, p):
        src = lax.rem(me + o, n)
        sender = lax.rem(dp + p, nd)
        ref = w1s.at[src, at_rows(sender * half, half)]
        return pltpu.make_async_remote_copy(
            src_ref=ref, dst_ref=ref, send_sem=dp_send.at[src, p], recv_sem=dp_recv.at[src, sender],
            device_id={"dp": sender})

    start_own(make_x)
    for o in range(1, n):
        w1_copy(o).start()

    def x_landed(src):
        for o in range(1, m):
            xy_copy(src, o).start()

    relay(make_x, x_landed)
    for o in range(1, n):
        w1_landed(o).wait_recv()
        for p in range(1, nd):
            dp_copy(o, p).start()
    own_w1.wait()
    own_w2.wait()
    for o in range(1, n):
        for q in range(1, m):
            xy_landed(lax.rem(me + o, n), q).wait_recv()
        for p in range(1, nd):
            dp_landed(o, p).wait_recv()

    def make_h(b):
        return functools.partial(
            line, lambda s: h.at[s, at_rows(b * block, block)],
            lambda s: h_r.at[b, s], lambda s: h_l.at[b, s], lambda s: h_recv.at[b, s])

    def rs_copy(b, o):
        to = lax.rem(cb + o, m)
        return pltpu.make_async_remote_copy(
            src_ref=rs_src.at[b, at_rows(to * rows, rows)], dst_ref=rs_recv.at[b, cb],
            send_sem=rs_send.at[b, o], recv_sem=rs_rcv.at[b, cb], device_id={"cb": to})

    def rs_landed(b, o):
        sender = lax.rem(cb + o, m)
        ref = rs_recv.at[b, sender]
        return pltpu.make_async_remote_copy(
            src_ref=ref, dst_ref=ref, send_sem=rs_send.at[b, o], recv_sem=rs_rcv.at[b, sender],
            device_id={"cb": sender})

    def st_copy(b, o):
        return pltpu.make_async_remote_copy(
            src_ref=st_src.at[b], dst_ref=st_recv.at[b, me],
            send_sem=st_send.at[b, o], recv_sem=st_rcv.at[b, me],
            device_id={"ra": lax.rem(me + o, n)})

    def st_landed(b, o):
        sender = lax.rem(me + o, n)
        ref = st_recv.at[b, sender]
        return pltpu.make_async_remote_copy(
            src_ref=ref, dst_ref=ref, send_sem=st_send.at[b, o], recv_sem=st_rcv.at[b, sender],
            device_id={"ra": sender})

    def fin_copy(b, o):
        ref = fin.at[at_rows(b * block + cb * rows, rows)]
        return pltpu.make_async_remote_copy(
            src_ref=ref, dst_ref=ref, send_sem=fin_send.at[b, o], recv_sem=fin_rcv.at[b, cb],
            device_id={"cb": lax.rem(cb + o, m)})

    def fin_landed(b, o):
        sender = lax.rem(cb + o, m)
        ref = fin.at[at_rows(b * block + sender * rows, rows)]
        return pltpu.make_async_remote_copy(
            src_ref=ref, dst_ref=ref, send_sem=fin_send.at[b, o], recv_sem=fin_rcv.at[b, sender],
            device_id={"cb": sender})

    def up(b):
        here = at_rows(b * block, block)

        @pl.loop(0, fs // tile)
        def _(t):
            cols = at_rows(t * tile, tile)
            acc = jnp.dot(xall[0, here, :], w1s[0, :, cols], preferred_element_type=jnp.float32)
            for k in range(1, n):
                acc += jnp.dot(xall[k, here, :], w1s[k, :, cols], preferred_element_type=jnp.float32)
            h[me, here, cols] = jnp.square(jnp.maximum(acc, 0.0)).astype(jnp.bfloat16)
        start_own(make_h(b))

    def down(b):
        here = at_rows(b * block, block)
        relay(make_h(b), lambda src: None)

        @pl.loop(0, dl // tile)
        def _(t):
            cols = at_rows(t * tile, tile)
            acc = jnp.dot(h[0, here, :], w2[pl.ds(0, fs), cols], preferred_element_type=jnp.float32)
            for k in range(1, n):
                acc += jnp.dot(h[k, here, :], w2[pl.ds(k * fs, fs), cols],
                               preferred_element_type=jnp.float32)
            part[:, cols] = acc
            rs_src[b, :, cols] = acc.astype(jnp.bfloat16)
        for o in range(1, m):
            rs_copy(b, o).start()
        mixed[b] = part[at_rows(cb * rows, rows), :] + residual_scale * xall[
            me, at_rows(b * block + cb * rows, rows), :].astype(jnp.float32)

    def reduce(b):
        total = mixed[b]
        for o in range(1, m):
            rs_landed(b, o).wait_recv()
            total += rs_recv[b, lax.rem(cb + o, m)].astype(jnp.float32)
        mixed[b] = total
        lane = lax.broadcasted_iota(jnp.int32, (rows, 128), 1)
        st_src[b] = jnp.where(
            lane < 64, jnp.sum(total, axis=1, keepdims=True),
            jnp.sum(total * total, axis=1, keepdims=True))
        for o in range(1, n):
            st_copy(b, o).start()

    def finish(b):
        sums = st_src[b]
        for o in range(1, n):
            st_landed(b, o).wait_recv()
            sums += st_recv[b, lax.rem(me + o, n)]
        mean = sums[:, 0:1] / width
        spread = sums[:, 64:65] / width - mean * mean
        fin[at_rows(b * block + cb * rows, rows), :] = (
            (mixed[b] - mean) * lax.rsqrt(spread + norm_eps) * gain_ref[...] + bias_ref[...]
        ).astype(jnp.bfloat16)
        for o in range(1, m):
            fin_copy(b, o).start()

    @pl.loop(0, blocks + lookahead + 2)
    def _(step):
        for lag, stage in ((0, up), (lookahead, down), (lookahead + 1, reduce),
                           (lookahead + 2, finish)):
            @pl.when((step >= lag) & (step < blocks + lag))
            def _():
                stage(step - lag)

    @pl.loop(0, blocks)
    def _(b):
        for o in range(1, m):
            fin_landed(b, o).wait_recv()
    out = pltpu.make_async_copy(fin, o_hbm, loc_sem.at[3])
    out.start()
    line_sent(make_x)
    for o in range(1, n):
        w1_copy(o).wait_send()
        for q in range(1, m):
            xy_copy(lax.rem(me + o, n), q).wait_send()
        for p in range(1, nd):
            dp_copy(o, p).wait_send()

    @pl.loop(0, blocks)
    def _(b):
        line_sent(make_h(b))
        for o in range(1, m):
            rs_copy(b, o).wait_send()
            fin_copy(b, o).wait_send()
        for o in range(1, n):
            st_copy(b, o).wait_send()
    out.wait()


def feed_forward(normed, up_weight, down_weight, gain_out, bias_out):
    n, m, nd = lax.axis_size("ra"), lax.axis_size("cb"), lax.axis_size("dp")
    tokens, dl = normed.shape
    fl = up_weight.shape[1]
    fs = fl // n
    block = math.gcd(tokens, 256)
    blocks = tokens // block
    rows = block // m
    dma = pltpu.SemaphoreType.DMA
    bf16, f32 = jnp.bfloat16, jnp.float32
    hbm = pl.BlockSpec(memory_space=pl.ANY)
    vmem = pl.BlockSpec(memory_space=pltpu.VMEM)
    return pl.pallas_call(
        functools.partial(kernel, n, m, nd, block),
        out_shape=jax.ShapeDtypeStruct((tokens, dl), bf16),
        in_specs=[hbm, hbm, hbm, vmem, vmem],
        out_specs=hbm,
        scratch_shapes=[
            pltpu.VMEM((n, tokens, dl), bf16),
            pltpu.VMEM((n, dl, fs), bf16),
            pltpu.VMEM((n, tokens, fs), bf16),
            pltpu.VMEM((fl, dl), bf16),
            pltpu.VMEM((block, dl), f32),
            pltpu.VMEM((blocks, block, dl), bf16),
            pltpu.VMEM((blocks, m, rows, dl), bf16),
            pltpu.VMEM((blocks, rows, dl), f32),
            pltpu.VMEM((blocks, rows, 128), f32),
            pltpu.VMEM((blocks, n, rows, 128), f32),
            pltpu.VMEM((tokens, dl), bf16),
            dma((4,)), dma((n,)), dma((n,)), dma((n, nd)), dma((n, nd)),
            dma((n,)), dma((n,)), dma((n,)), dma((n, m)), dma((n, m)),
            dma((blocks, n)), dma((blocks, n)), dma((blocks, n)),
            dma((blocks, m)), dma((blocks, m)), dma((blocks, n)), dma((blocks, n)),
            dma((blocks, m)), dma((blocks, m)),
        ],
        compiler_params=pltpu.CompilerParams(
            collective_id=0, has_side_effects=True, vmem_limit_bytes=66 * 1000 * 1000),
    )(normed, up_weight, down_weight, gain_out.reshape(1, dl), bias_out.reshape(1, dl))


def per_device(carried, branch_in, gain_in, bias_in, up_weight, down_weight, gain_out, bias_out):
    width = carried.shape[1] * lax.axis_size("ra")
    mixed_in = residual_scale * carried.astype(jnp.float32) + branch_in.astype(jnp.float32)
    totals, squares = lax.psum(
        (jnp.sum(mixed_in, axis=1), jnp.sum(mixed_in * mixed_in, axis=1)), "ra"
    )
    mean = totals[:, None] / width
    spread = squares[:, None] / width - mean * mean
    normed = ((mixed_in - mean) * lax.rsqrt(spread + norm_eps) * gain_in + bias_in).astype(
        jnp.bfloat16)
    return feed_forward(normed, up_weight, down_weight, gain_out, bias_out)


def solution(mesh):
    in_specs = (
        P("dp", "ra"),
        P("dp", "ra"),
        P("ra"),
        P("ra"),
        P("ra", "cb"),
        P("cb", "ra"),
        P("ra"),
        P("ra"),
    )
    out_specs = P("dp", "ra")
    return jax.shard_map(
        per_device, mesh=mesh, in_specs=in_specs, out_specs=out_specs, check_vma=False
    )
```

```python
import functools
import math

import jax
import jax.numpy as jnp
from jax import lax
from jax.experimental import pallas as pl
from jax.experimental.pallas import tpu as pltpu
from jax.sharding import PartitionSpec as P

residual_scale = 2.0**0.25
norm_eps = 1e-05
lookahead = 2


def kernel(n, m, nd, block, carried_hbm, branch_hbm, w1_hbm, w2_hbm, gain_in_ref, bias_in_ref,
           gain_ref, bias_ref, o_hbm, s1_src, s1_recv, s1_tot, s1_send, s1_rcv, xall, w1s, h, w2, part, rs_src, rs_recv, mixed, st_src, st_recv, fin,
           loc_sem, w1_send, w1_recv, dp_send, dp_recv, xz_r, xz_l, xz_recv,
           xy_send, xy_recv, h_r, h_l, h_recv, rs_send, rs_rcv, st_send, st_rcv,
           fin_send, fin_rcv):
    me, cb, dp = lax.axis_index("ra"), lax.axis_index("cb"), lax.axis_index("dp")
    _, tokens, dl = xall.shape
    fs = w1s.shape[2]
    blocks = tokens // block
    quarter = tokens // m
    rows = block // m
    half = dl // nd
    pieces = w1_send.shape[1]
    piece = half // pieces
    width = n * dl
    tile = math.gcd(256, math.gcd(fs, dl))

    barrier = pltpu.get_barrier_semaphore()
    for o in range(1, n):
        pl.semaphore_signal(barrier, inc=1, device_id={"ra": lax.rem(me + o, n)})
    for o in range(1, m):
        pl.semaphore_signal(barrier, inc=1, device_id={"cb": lax.rem(cb + o, m)})
    for o in range(1, nd):
        pl.semaphore_signal(barrier, inc=1, device_id={"dp": lax.rem(dp + o, nd)})

    own_carried = pltpu.make_async_copy(carried_hbm, fin, loc_sem.at[0])
    own_branch = pltpu.make_async_copy(branch_hbm, rs_src, loc_sem.at[4])
    own_w1 = pltpu.make_async_copy(
        w1_hbm.at[:, pl.ds(pl.multiple_of(me * fs, fs), fs)], w1s.at[me], loc_sem.at[1])
    own_w2 = pltpu.make_async_copy(w2_hbm, w2, loc_sem.at[2])
    own_carried.start()
    own_branch.start()
    own_w1.start()
    own_w2.start()
    pl.semaphore_wait(barrier, n + m + nd - 3)

    def at_rows(start, size):
        return pl.ds(pl.multiple_of(start, size), size)

    def line(ref_of, right_sem, left_sem, recv_sem, src, to_right):
        ref = ref_of(src)
        return pltpu.make_async_remote_copy(
            src_ref=ref, dst_ref=ref,
            send_sem=(right_sem if to_right else left_sem)(src),
            recv_sem=recv_sem(src),
            device_id={"ra": jnp.minimum(me + 1, n - 1) if to_right else jnp.maximum(me - 1, 0)})

    def start_own(make):
        @pl.when(me + 1 < n)
        def _():
            make(me, True).start()

        @pl.when(me >= 1)
        def _():
            make(me, False).start()

    def relay(make, landed, between=None):
        for s in range(1, n):
            @pl.when(me - s >= 0)
            def _():
                make(me - s, True).wait_recv()

                @pl.when(me + 1 < n)
                def _():
                    make(me - s, True).start()
                landed(me - s)

            @pl.when(me + s < n)
            def _():
                make(me + s, False).wait_recv()

                @pl.when(me >= 1)
                def _():
                    make(me + s, False).start()
                landed(me + s)
            if between is not None:
                between(s)

    def line_sent(make):
        for s in range(n):
            @pl.when((me - s >= 0) & (me + 1 < n))
            def _():
                make(me - s, True).wait_send()

            @pl.when((me + s < n) & (me >= 1))
            def _():
                make(me + s, False).wait_send()

    make_x = functools.partial(
        line, lambda s: xall.at[s, at_rows(cb * quarter, quarter)],
        lambda s: xz_r.at[s], lambda s: xz_l.at[s], lambda s: xz_recv.at[s])

    def xy_copy(src, o):
        ref = xall.at[src, at_rows(cb * quarter, quarter)]
        return pltpu.make_async_remote_copy(
            src_ref=ref, dst_ref=ref, send_sem=xy_send.at[src, o], recv_sem=xy_recv.at[src, cb],
            device_id={"cb": lax.rem(cb + o, m)})

    def xy_landed(src, o):
        sender = lax.rem(cb + o, m)
        ref = xall.at[src, at_rows(sender * quarter, quarter)]
        return pltpu.make_async_remote_copy(
            src_ref=ref, dst_ref=ref, send_sem=xy_send.at[src, o], recv_sem=xy_recv.at[src, sender],
            device_id={"cb": sender})

    def w1_copy(o, p):
        to = lax.rem(me + o, n)
        here = at_rows(dp * half + p * piece, piece)
        return pltpu.make_async_remote_copy(
            src_ref=w1_hbm.at[here, pl.ds(pl.multiple_of(to * fs, fs), fs)],
            dst_ref=w1s.at[me, here],
            send_sem=w1_send.at[to, p], recv_sem=w1_recv.at[me, p], device_id={"ra": to})

    def w1_landed(o, p):
        src = lax.rem(me + o, n)
        ref = w1s.at[src, at_rows(dp * half + p * piece, piece)]
        return pltpu.make_async_remote_copy(
            src_ref=ref, dst_ref=ref, send_sem=w1_send.at[src, p], recv_sem=w1_recv.at[src, p],
            device_id={"ra": src})

    def w1_pieces(p):
        if p < pieces:
            for o in range(1, n):
                w1_copy(o, p).start()

    def s1_copy(o):
        return pltpu.make_async_remote_copy(
            src_ref=s1_src, dst_ref=s1_recv.at[me], send_sem=s1_send.at[o],
            recv_sem=s1_rcv.at[me], device_id={"ra": lax.rem(me + o, n)})

    def s1_landed(o):
        sender = lax.rem(me + o, n)
        ref = s1_recv.at[sender]
        return pltpu.make_async_remote_copy(
            src_ref=ref, dst_ref=ref, send_sem=s1_send.at[o], recv_sem=s1_rcv.at[sender],
            device_id={"ra": sender})

    chunks = tokens // 128

    def mixed_in(here):
        return residual_scale * fin[here, :].astype(jnp.float32) + rs_src[here, :].astype(
            jnp.float32)

    def sums_of(total):
        lane = lax.broadcasted_iota(jnp.int32, (total.shape[0], 128), 1)
        tile = jnp.where(
            lane < 64, jnp.sum(total, axis=1, keepdims=True),
            jnp.sum(total * total, axis=1, keepdims=True))
        if total.shape[0] < 128:
            tile = jnp.concatenate([tile] * (128 // total.shape[0]), axis=0)
        return tile.T

    def column(row):
        return jnp.broadcast_to(row, (128, 128)).T[:, 0:1]

    def dp_copy(o, p):
        src = lax.rem(me + o, n)
        ref = w1s.at[src, at_rows(dp * half, half)]
        return pltpu.make_async_remote_copy(
            src_ref=ref, dst_ref=ref, send_sem=dp_send.at[src, p], recv_sem=dp_recv.at[src, dp],
            device_id={"dp": lax.rem(dp + p, nd)})

    def dp_landed(o, p):
        src = lax.rem(me + o, n)
        sender = lax.rem(dp + p, nd)
        ref = w1s.at[src, at_rows(sender * half, half)]
        return pltpu.make_async_remote_copy(
            src_ref=ref, dst_ref=ref, send_sem=dp_send.at[src, p], recv_sem=dp_recv.at[src, sender],
            device_id={"dp": sender})

    w1_pieces(0)
    own_carried.wait()
    own_branch.wait()

    @pl.loop(0, chunks)
    def _(c):
        sums = sums_of(mixed_in(at_rows(c * 128, 128)))
        s1_src[pl.ds(c, 1), :] = sums[0:1, :]
        s1_src[pl.ds(chunks + c, 1), :] = sums[64:65, :]
    for o in range(1, n):
        s1_copy(o).start()
    s1_tot[...] = s1_src[...]
    for o in range(1, n):
        s1_landed(o).wait_recv()
        s1_tot[...] += s1_recv[lax.rem(me + o, n)]

    @pl.loop(0, chunks)
    def _(c):
        here = at_rows(c * 128, 128)
        mean_row = s1_tot[pl.ds(c, 1), :] / width
        scale_row = lax.rsqrt(s1_tot[pl.ds(chunks + c, 1), :] / width - mean_row * mean_row + norm_eps)
        xall[me, here, :] = (
            (mixed_in(here) - column(mean_row)) * column(scale_row) * gain_in_ref[...]
            + bias_in_ref[...]
        ).astype(jnp.bfloat16)
    start_own(make_x)
    w1_pieces(1)

    def x_landed(src):
        for o in range(1, m):
            xy_copy(src, o).start()

    relay(make_x, x_landed, lambda s: w1_pieces(s + 1))
    for p in range(n + 1, pieces):
        w1_pieces(p)
    for o in range(1, n):
        for p in range(pieces):
            w1_landed(o, p).wait_recv()
        for p in range(1, nd):
            dp_copy(o, p).start()
    own_w1.wait()
    own_w2.wait()
    for o in range(1, n):
        for q in range(1, m):
            xy_landed(lax.rem(me + o, n), q).wait_recv()
        for p in range(1, nd):
            dp_landed(o, p).wait_recv()

    def make_h(b):
        return functools.partial(
            line, lambda s: h.at[s, at_rows(b * block, block)],
            lambda s: h_r.at[b, s], lambda s: h_l.at[b, s], lambda s: h_recv.at[b, s])

    def rs_copy(b, o):
        to = lax.rem(cb + o, m)
        return pltpu.make_async_remote_copy(
            src_ref=rs_src.at[at_rows(b * block + to * rows, rows)], dst_ref=rs_recv.at[b, cb],
            send_sem=rs_send.at[b, o], recv_sem=rs_rcv.at[b, cb], device_id={"cb": to})

    def rs_landed(b, o):
        sender = lax.rem(cb + o, m)
        ref = rs_recv.at[b, sender]
        return pltpu.make_async_remote_copy(
            src_ref=ref, dst_ref=ref, send_sem=rs_send.at[b, o], recv_sem=rs_rcv.at[b, sender],
            device_id={"cb": sender})

    def st_copy(b, o):
        return pltpu.make_async_remote_copy(
            src_ref=st_src.at[b], dst_ref=st_recv.at[b, me],
            send_sem=st_send.at[b, o], recv_sem=st_rcv.at[b, me],
            device_id={"ra": lax.rem(me + o, n)})

    def st_landed(b, o):
        sender = lax.rem(me + o, n)
        ref = st_recv.at[b, sender]
        return pltpu.make_async_remote_copy(
            src_ref=ref, dst_ref=ref, send_sem=st_send.at[b, o], recv_sem=st_rcv.at[b, sender],
            device_id={"ra": sender})

    def fin_copy(b, o):
        ref = fin.at[at_rows(b * block + cb * rows, rows)]
        return pltpu.make_async_remote_copy(
            src_ref=ref, dst_ref=ref, send_sem=fin_send.at[b, o], recv_sem=fin_rcv.at[b, cb],
            device_id={"cb": lax.rem(cb + o, m)})

    def fin_landed(b, o):
        sender = lax.rem(cb + o, m)
        ref = fin.at[at_rows(b * block + sender * rows, rows)]
        return pltpu.make_async_remote_copy(
            src_ref=ref, dst_ref=ref, send_sem=fin_send.at[b, o], recv_sem=fin_rcv.at[b, sender],
            device_id={"cb": sender})

    def up(b):
        here = at_rows(b * block, block)

        @pl.loop(0, fs // tile)
        def _(t):
            cols = at_rows(t * tile, tile)
            acc = jnp.dot(xall[0, here, :], w1s[0, :, cols], preferred_element_type=jnp.float32)
            for k in range(1, n):
                acc += jnp.dot(xall[k, here, :], w1s[k, :, cols], preferred_element_type=jnp.float32)
            h[me, here, cols] = jnp.square(jnp.maximum(acc, 0.0)).astype(jnp.bfloat16)
        start_own(make_h(b))

    def down(b):
        here = at_rows(b * block, block)
        relay(make_h(b), lambda src: None)

        @pl.loop(0, dl // tile)
        def _(t):
            cols = at_rows(t * tile, tile)
            acc = jnp.dot(h[0, here, :], w2[pl.ds(0, fs), cols], preferred_element_type=jnp.float32)
            for k in range(1, n):
                acc += jnp.dot(h[k, here, :], w2[pl.ds(k * fs, fs), cols],
                               preferred_element_type=jnp.float32)
            part[:, cols] = acc
            rs_src[here, cols] = acc.astype(jnp.bfloat16)
        for o in range(1, m):
            rs_copy(b, o).start()
        mixed[b] = part[at_rows(cb * rows, rows), :] + residual_scale * xall[
            me, at_rows(b * block + cb * rows, rows), :].astype(jnp.float32)

    def reduce(b):
        total = mixed[b]
        for o in range(1, m):
            rs_landed(b, o).wait_recv()
            total += rs_recv[b, lax.rem(cb + o, m)].astype(jnp.float32)
        mixed[b] = total
        sums = sums_of(total)
        st_src[b] = jnp.concatenate([sums[0:4, :], sums[64:68, :]], axis=0)
        for o in range(1, n):
            st_copy(b, o).start()

    def finish(b):
        sums = st_src[b]
        for o in range(1, n):
            st_landed(b, o).wait_recv()
            sums += st_recv[b, lax.rem(me + o, n)]
        mean_row = sums[0:1, :] / width
        scale_row = lax.rsqrt(sums[4:5, :] / width - mean_row * mean_row + norm_eps)
        mean, scale = column(mean_row)[0:rows], column(scale_row)[0:rows]
        fin[at_rows(b * block + cb * rows, rows), :] = (
            (mixed[b] - mean) * scale * gain_ref[...] + bias_ref[...]
        ).astype(jnp.bfloat16)
        for o in range(1, m):
            fin_copy(b, o).start()

    @pl.loop(0, blocks + lookahead + 2)
    def _(step):
        for lag, stage in ((0, up), (lookahead, down), (lookahead + 1, reduce),
                           (lookahead + 2, finish)):
            @pl.when((step >= lag) & (step < blocks + lag))
            def _():
                stage(step - lag)

    @pl.loop(0, blocks)
    def _(b):
        for o in range(1, m):
            fin_landed(b, o).wait_recv()
    out = pltpu.make_async_copy(fin, o_hbm, loc_sem.at[3])
    out.start()
    line_sent(make_x)
    for o in range(1, n):
        s1_copy(o).wait_send()
        for p in range(pieces):
            w1_copy(o, p).wait_send()
        for q in range(1, m):
            xy_copy(lax.rem(me + o, n), q).wait_send()
        for p in range(1, nd):
            dp_copy(o, p).wait_send()

    @pl.loop(0, blocks)
    def _(b):
        line_sent(make_h(b))
        for o in range(1, m):
            rs_copy(b, o).wait_send()
            fin_copy(b, o).wait_send()
        for o in range(1, n):
            st_copy(b, o).wait_send()
    out.wait()


def per_device(carried, branch_in, gain_in, bias_in, up_weight, down_weight, gain_out, bias_out):
    n, m, nd = lax.axis_size("ra"), lax.axis_size("cb"), lax.axis_size("dp")
    tokens, dl = carried.shape
    fl = up_weight.shape[1]
    fs = fl // n
    block = math.gcd(tokens, 256)
    blocks = tokens // block
    rows = block // m
    pieces = 4
    chunk_rows = -(-2 * (tokens // 128) // 8) * 8
    dma = pltpu.SemaphoreType.DMA
    bf16, f32 = jnp.bfloat16, jnp.float32
    hbm = pl.BlockSpec(memory_space=pl.ANY)
    vmem = pl.BlockSpec(memory_space=pltpu.VMEM)
    return pl.pallas_call(
        functools.partial(kernel, n, m, nd, block),
        out_shape=jax.ShapeDtypeStruct((tokens, dl), bf16),
        in_specs=[hbm, hbm, hbm, hbm, vmem, vmem, vmem, vmem],
        out_specs=hbm,
        scratch_shapes=[
            pltpu.VMEM((chunk_rows, 128), f32),
            pltpu.VMEM((n, chunk_rows, 128), f32),
            pltpu.VMEM((chunk_rows, 128), f32),
            dma((n,)), dma((n,)),
            pltpu.VMEM((n, tokens, dl), bf16),
            pltpu.VMEM((n, dl, fs), bf16),
            pltpu.VMEM((n, tokens, fs), bf16),
            pltpu.VMEM((fl, dl), bf16),
            pltpu.VMEM((block, dl), f32),
            pltpu.VMEM((tokens, dl), bf16),
            pltpu.VMEM((blocks, m, rows, dl), bf16),
            pltpu.VMEM((blocks, rows, dl), f32),
            pltpu.VMEM((blocks, 8, 128), f32),
            pltpu.VMEM((blocks, n, 8, 128), f32),
            pltpu.VMEM((tokens, dl), bf16),
            dma((5,)), dma((n, pieces)), dma((n, pieces)), dma((n, nd)), dma((n, nd)),
            dma((n,)), dma((n,)), dma((n,)), dma((n, m)), dma((n, m)),
            dma((blocks, n)), dma((blocks, n)), dma((blocks, n)),
            dma((blocks, m)), dma((blocks, m)), dma((blocks, n)), dma((blocks, n)),
            dma((blocks, m)), dma((blocks, m)),
        ],
        compiler_params=pltpu.CompilerParams(
            collective_id=0, has_side_effects=True, vmem_limit_bytes=66 * 1000 * 1000),
    )(carried, branch_in, up_weight, down_weight, gain_in.reshape(1, dl), bias_in.reshape(1, dl),
      gain_out.reshape(1, dl), bias_out.reshape(1, dl))


def solution(mesh):
    in_specs = (
        P("dp", "ra"),
        P("dp", "ra"),
        P("ra"),
        P("ra"),
        P("ra", "cb"),
        P("cb", "ra"),
        P("ra"),
        P("ra"),
    )
    out_specs = P("dp", "ra")
    return jax.shard_map(
        per_device, mesh=mesh, in_specs=in_specs, out_specs=out_specs, check_vma=False
    )
```

```python
import functools
import math

import jax
import jax.numpy as jnp
from jax import lax
from jax.experimental import pallas as pl
from jax.experimental.pallas import tpu as pltpu
from jax.sharding import PartitionSpec as P

residual_scale = 2.0**0.25
norm_eps = 1e-05
lookahead = 4


def kernel(n, m, nd, block, carried_hbm, branch_hbm, w1_hbm, w2_hbm, gain_in_ref, bias_in_ref,
           gain_ref, bias_ref, o_hbm, s1_src, s1_recv, s1_tot, s1_send, s1_rcv, xall, w1s, h, w2, part, rs_src, rs_recv, mixed, st_src, st_recv, fin,
           loc_sem, w1_send, w1_recv, dp_send, dp_recv, xz_r, xz_l, xz_recv,
           xy_send, xy_recv, h_r, h_l, h_recv, rs_send, rs_rcv, st_send, st_rcv,
           fin_send, fin_rcv):
    me, cb, dp = lax.axis_index("ra"), lax.axis_index("cb"), lax.axis_index("dp")
    _, tokens, dl = xall.shape
    fs = w1s.shape[2]
    blocks = tokens // block
    quarter = tokens // m
    rows = block // m
    half = dl // nd
    pieces = w1_send.shape[1]
    piece = half // pieces
    width = n * dl
    tile = math.gcd(256, math.gcd(fs, dl))

    barrier = pltpu.get_barrier_semaphore()
    for o in range(1, n):
        pl.semaphore_signal(barrier, inc=1, device_id={"ra": lax.rem(me + o, n)})
    for o in range(1, m):
        pl.semaphore_signal(barrier, inc=1, device_id={"cb": lax.rem(cb + o, m)})
    for o in range(1, nd):
        pl.semaphore_signal(barrier, inc=1, device_id={"dp": lax.rem(dp + o, nd)})

    own_carried = pltpu.make_async_copy(carried_hbm, fin, loc_sem.at[0])
    own_branch = pltpu.make_async_copy(branch_hbm, rs_src, loc_sem.at[4])
    own_w1 = pltpu.make_async_copy(
        w1_hbm.at[:, pl.ds(pl.multiple_of(me * fs, fs), fs)], w1s.at[me], loc_sem.at[1])
    own_w2 = pltpu.make_async_copy(w2_hbm, w2, loc_sem.at[2])
    own_carried.start()
    own_branch.start()
    own_w1.start()
    own_w2.start()
    pl.semaphore_wait(barrier, n + m + nd - 3)

    def at_rows(start, size):
        return pl.ds(pl.multiple_of(start, size), size)

    def line(ref_of, right_sem, left_sem, recv_sem, src, to_right):
        ref = ref_of(src)
        return pltpu.make_async_remote_copy(
            src_ref=ref, dst_ref=ref,
            send_sem=(right_sem if to_right else left_sem)(src),
            recv_sem=recv_sem(src),
            device_id={"ra": jnp.minimum(me + 1, n - 1) if to_right else jnp.maximum(me - 1, 0)})

    def start_own(make):
        @pl.when(me + 1 < n)
        def _():
            make(me, True).start()

        @pl.when(me >= 1)
        def _():
            make(me, False).start()

    def relay(make, landed, between=None):
        for s in range(1, n):
            @pl.when(me - s >= 0)
            def _():
                make(me - s, True).wait_recv()

                @pl.when(me + 1 < n)
                def _():
                    make(me - s, True).start()
                landed(me - s)

            @pl.when(me + s < n)
            def _():
                make(me + s, False).wait_recv()

                @pl.when(me >= 1)
                def _():
                    make(me + s, False).start()
                landed(me + s)
            if between is not None:
                between(s)

    def line_sent(make):
        for s in range(n):
            @pl.when((me - s >= 0) & (me + 1 < n))
            def _():
                make(me - s, True).wait_send()

            @pl.when((me + s < n) & (me >= 1))
            def _():
                make(me + s, False).wait_send()

    make_x = functools.partial(
        line, lambda s: xall.at[s, at_rows(cb * quarter, quarter)],
        lambda s: xz_r.at[s], lambda s: xz_l.at[s], lambda s: xz_recv.at[s])

    def xy_copy(src, o):
        ref = xall.at[src, at_rows(cb * quarter, quarter)]
        return pltpu.make_async_remote_copy(
            src_ref=ref, dst_ref=ref, send_sem=xy_send.at[src, o], recv_sem=xy_recv.at[src, cb],
            device_id={"cb": lax.rem(cb + o, m)})

    def xy_landed(src, o):
        sender = lax.rem(cb + o, m)
        ref = xall.at[src, at_rows(sender * quarter, quarter)]
        return pltpu.make_async_remote_copy(
            src_ref=ref, dst_ref=ref, send_sem=xy_send.at[src, o], recv_sem=xy_recv.at[src, sender],
            device_id={"cb": sender})

    def w1_copy(o, p):
        to = lax.rem(me + o, n)
        here = at_rows(dp * half + p * piece, piece)
        return pltpu.make_async_remote_copy(
            src_ref=w1_hbm.at[here, pl.ds(pl.multiple_of(to * fs, fs), fs)],
            dst_ref=w1s.at[me, here],
            send_sem=w1_send.at[to, p], recv_sem=w1_recv.at[me, p], device_id={"ra": to})

    def w1_landed(o, p):
        src = lax.rem(me + o, n)
        ref = w1s.at[src, at_rows(dp * half + p * piece, piece)]
        return pltpu.make_async_remote_copy(
            src_ref=ref, dst_ref=ref, send_sem=w1_send.at[src, p], recv_sem=w1_recv.at[src, p],
            device_id={"ra": src})

    def w1_pieces(p):
        if p < pieces:
            for o in range(1, n):
                w1_copy(o, p).start()

    def s1_copy(o):
        return pltpu.make_async_remote_copy(
            src_ref=s1_src, dst_ref=s1_recv.at[me], send_sem=s1_send.at[o],
            recv_sem=s1_rcv.at[me], device_id={"ra": lax.rem(me + o, n)})

    def s1_landed(o):
        sender = lax.rem(me + o, n)
        ref = s1_recv.at[sender]
        return pltpu.make_async_remote_copy(
            src_ref=ref, dst_ref=ref, send_sem=s1_send.at[o], recv_sem=s1_rcv.at[sender],
            device_id={"ra": sender})

    chunks = tokens // 128

    def mixed_in(here):
        return residual_scale * fin[here, :].astype(jnp.float32) + rs_src[here, :].astype(
            jnp.float32)

    def sums_of(total):
        lane = lax.broadcasted_iota(jnp.int32, (total.shape[0], 128), 1)
        tile = jnp.where(
            lane < 64, jnp.sum(total, axis=1, keepdims=True),
            jnp.sum(total * total, axis=1, keepdims=True))
        if total.shape[0] < 128:
            tile = jnp.concatenate([tile] * (128 // total.shape[0]), axis=0)
        return tile.T

    def column(row):
        return jnp.broadcast_to(row, (128, 128)).T[:, 0:1]

    def dp_copy(o, p):
        src = lax.rem(me + o, n)
        ref = w1s.at[src, at_rows(dp * half, half)]
        return pltpu.make_async_remote_copy(
            src_ref=ref, dst_ref=ref, send_sem=dp_send.at[src, p], recv_sem=dp_recv.at[src, dp],
            device_id={"dp": lax.rem(dp + p, nd)})

    def dp_landed(o, p):
        src = lax.rem(me + o, n)
        sender = lax.rem(dp + p, nd)
        ref = w1s.at[src, at_rows(sender * half, half)]
        return pltpu.make_async_remote_copy(
            src_ref=ref, dst_ref=ref, send_sem=dp_send.at[src, p], recv_sem=dp_recv.at[src, sender],
            device_id={"dp": sender})

    w1_pieces(0)
    own_carried.wait()
    own_branch.wait()

    @pl.loop(0, chunks)
    def _(c):
        sums = sums_of(mixed_in(at_rows(c * 128, 128)))
        s1_src[pl.ds(c, 1), :] = sums[0:1, :]
        s1_src[pl.ds(chunks + c, 1), :] = sums[64:65, :]
    for o in range(1, n):
        s1_copy(o).start()
    s1_tot[...] = s1_src[...]
    for o in range(1, n):
        s1_landed(o).wait_recv()
        s1_tot[...] += s1_recv[lax.rem(me + o, n)]

    @pl.loop(0, chunks)
    def _(c):
        here = at_rows(c * 128, 128)
        mean_row = s1_tot[pl.ds(c, 1), :] / width
        scale_row = lax.rsqrt(s1_tot[pl.ds(chunks + c, 1), :] / width - mean_row * mean_row + norm_eps)
        xall[me, here, :] = (
            (mixed_in(here) - column(mean_row)) * column(scale_row) * gain_in_ref[...]
            + bias_in_ref[...]
        ).astype(jnp.bfloat16)
    start_own(make_x)
    w1_pieces(1)

    def x_landed(src):
        for o in range(1, m):
            xy_copy(src, o).start()

    relay(make_x, x_landed, lambda s: w1_pieces(s + 1))
    for p in range(n + 1, pieces):
        w1_pieces(p)
    for o in range(1, n):
        for p in range(pieces):
            w1_landed(o, p).wait_recv()
        for p in range(1, nd):
            dp_copy(o, p).start()
    own_w1.wait()
    own_w2.wait()
    for o in range(1, n):
        for q in range(1, m):
            xy_landed(lax.rem(me + o, n), q).wait_recv()
        for p in range(1, nd):
            dp_landed(o, p).wait_recv()

    def make_h(b):
        return functools.partial(
            line, lambda s: h.at[s, at_rows(b * block, block)],
            lambda s: h_r.at[b, s], lambda s: h_l.at[b, s], lambda s: h_recv.at[b, s])

    def rs_copy(b, o):
        to = lax.rem(cb + o, m)
        return pltpu.make_async_remote_copy(
            src_ref=rs_src.at[at_rows(b * block + to * rows, rows)], dst_ref=rs_recv.at[b, cb],
            send_sem=rs_send.at[b, o], recv_sem=rs_rcv.at[b, cb], device_id={"cb": to})

    def rs_landed(b, o):
        sender = lax.rem(cb + o, m)
        ref = rs_recv.at[b, sender]
        return pltpu.make_async_remote_copy(
            src_ref=ref, dst_ref=ref, send_sem=rs_send.at[b, o], recv_sem=rs_rcv.at[b, sender],
            device_id={"cb": sender})

    def st_copy(b, o):
        return pltpu.make_async_remote_copy(
            src_ref=st_src.at[b], dst_ref=st_recv.at[b, me],
            send_sem=st_send.at[b, o], recv_sem=st_rcv.at[b, me],
            device_id={"ra": lax.rem(me + o, n)})

    def st_landed(b, o):
        sender = lax.rem(me + o, n)
        ref = st_recv.at[b, sender]
        return pltpu.make_async_remote_copy(
            src_ref=ref, dst_ref=ref, send_sem=st_send.at[b, o], recv_sem=st_rcv.at[b, sender],
            device_id={"ra": sender})

    def fin_copy(b, o):
        ref = fin.at[at_rows(b * block + cb * rows, rows)]
        return pltpu.make_async_remote_copy(
            src_ref=ref, dst_ref=ref, send_sem=fin_send.at[b, o], recv_sem=fin_rcv.at[b, cb],
            device_id={"cb": lax.rem(cb + o, m)})

    def fin_landed(b, o):
        sender = lax.rem(cb + o, m)
        ref = fin.at[at_rows(b * block + sender * rows, rows)]
        return pltpu.make_async_remote_copy(
            src_ref=ref, dst_ref=ref, send_sem=fin_send.at[b, o], recv_sem=fin_rcv.at[b, sender],
            device_id={"cb": sender})

    def up(b):
        here = at_rows(b * block, block)

        @pl.loop(0, fs // tile)
        def _(t):
            cols = at_rows(t * tile, tile)
            acc = jnp.dot(xall[0, here, :], w1s[0, :, cols], preferred_element_type=jnp.float32)
            for k in range(1, n):
                acc += jnp.dot(xall[k, here, :], w1s[k, :, cols], preferred_element_type=jnp.float32)
            h[me, here, cols] = jnp.square(jnp.maximum(acc, 0.0)).astype(jnp.bfloat16)
        start_own(make_h(b))

    def down(b):
        here = at_rows(b * block, block)
        relay(make_h(b), lambda src: None)

        @pl.loop(0, dl // tile)
        def _(t):
            cols = at_rows(t * tile, tile)
            acc = jnp.dot(h[0, here, :], w2[pl.ds(0, fs), cols], preferred_element_type=jnp.float32)
            for k in range(1, n):
                acc += jnp.dot(h[k, here, :], w2[pl.ds(k * fs, fs), cols],
                               preferred_element_type=jnp.float32)
            part[:, cols] = acc
            rs_src[here, cols] = acc.astype(jnp.bfloat16)
        for o in range(1, m):
            rs_copy(b, o).start()
        mixed[b] = part[at_rows(cb * rows, rows), :] + residual_scale * xall[
            me, at_rows(b * block + cb * rows, rows), :].astype(jnp.float32)

    def reduce(b):
        total = mixed[b]
        for o in range(1, m):
            rs_landed(b, o).wait_recv()
            total += rs_recv[b, lax.rem(cb + o, m)].astype(jnp.float32)
        mixed[b] = total
        sums = sums_of(total)
        st_src[b] = jnp.concatenate([sums[0:4, :], sums[64:68, :]], axis=0)
        for o in range(1, n):
            st_copy(b, o).start()

    def finish(b):
        sums = st_src[b]
        for o in range(1, n):
            st_landed(b, o).wait_recv()
            sums += st_recv[b, lax.rem(me + o, n)]
        mean_row = sums[0:1, :] / width
        scale_row = lax.rsqrt(sums[4:5, :] / width - mean_row * mean_row + norm_eps)
        mean, scale = column(mean_row)[0:rows], column(scale_row)[0:rows]
        fin[at_rows(b * block + cb * rows, rows), :] = (
            (mixed[b] - mean) * scale * gain_ref[...] + bias_ref[...]
        ).astype(jnp.bfloat16)
        for o in range(1, m):
            fin_copy(b, o).start()

    @pl.loop(0, blocks + lookahead + 2)
    def _(step):
        for lag, stage in ((0, up), (lookahead, down), (lookahead + 1, reduce),
                           (lookahead + 2, finish)):
            @pl.when((step >= lag) & (step < blocks + lag))
            def _():
                stage(step - lag)

    @pl.loop(0, blocks)
    def _(b):
        for o in range(1, m):
            fin_landed(b, o).wait_recv()
    out = pltpu.make_async_copy(fin, o_hbm, loc_sem.at[3])
    out.start()
    line_sent(make_x)
    for o in range(1, n):
        s1_copy(o).wait_send()
        for p in range(pieces):
            w1_copy(o, p).wait_send()
        for q in range(1, m):
            xy_copy(lax.rem(me + o, n), q).wait_send()
        for p in range(1, nd):
            dp_copy(o, p).wait_send()

    @pl.loop(0, blocks)
    def _(b):
        line_sent(make_h(b))
        for o in range(1, m):
            rs_copy(b, o).wait_send()
            fin_copy(b, o).wait_send()
        for o in range(1, n):
            st_copy(b, o).wait_send()
    out.wait()


def per_device(carried, branch_in, gain_in, bias_in, up_weight, down_weight, gain_out, bias_out):
    n, m, nd = lax.axis_size("ra"), lax.axis_size("cb"), lax.axis_size("dp")
    tokens, dl = carried.shape
    fl = up_weight.shape[1]
    fs = fl // n
    block = math.gcd(tokens, 128)
    blocks = tokens // block
    rows = block // m
    pieces = 4
    chunk_rows = -(-2 * (tokens // 128) // 8) * 8
    dma = pltpu.SemaphoreType.DMA
    bf16, f32 = jnp.bfloat16, jnp.float32
    hbm = pl.BlockSpec(memory_space=pl.ANY)
    vmem = pl.BlockSpec(memory_space=pltpu.VMEM)
    return pl.pallas_call(
        functools.partial(kernel, n, m, nd, block),
        out_shape=jax.ShapeDtypeStruct((tokens, dl), bf16),
        in_specs=[hbm, hbm, hbm, hbm, vmem, vmem, vmem, vmem],
        out_specs=hbm,
        scratch_shapes=[
            pltpu.VMEM((chunk_rows, 128), f32),
            pltpu.VMEM((n, chunk_rows, 128), f32),
            pltpu.VMEM((chunk_rows, 128), f32),
            dma((n,)), dma((n,)),
            pltpu.VMEM((n, tokens, dl), bf16),
            pltpu.VMEM((n, dl, fs), bf16),
            pltpu.VMEM((n, tokens, fs), bf16),
            pltpu.VMEM((fl, dl), bf16),
            pltpu.VMEM((block, dl), f32),
            pltpu.VMEM((tokens, dl), bf16),
            pltpu.VMEM((blocks, m, rows, dl), bf16),
            pltpu.VMEM((blocks, rows, dl), f32),
            pltpu.VMEM((blocks, 8, 128), f32),
            pltpu.VMEM((blocks, n, 8, 128), f32),
            pltpu.VMEM((tokens, dl), bf16),
            dma((5,)), dma((n, pieces)), dma((n, pieces)), dma((n, nd)), dma((n, nd)),
            dma((n,)), dma((n,)), dma((n,)), dma((n, m)), dma((n, m)),
            dma((blocks, n)), dma((blocks, n)), dma((blocks, n)),
            dma((blocks, m)), dma((blocks, m)), dma((blocks, n)), dma((blocks, n)),
            dma((blocks, m)), dma((blocks, m)),
        ],
        compiler_params=pltpu.CompilerParams(
            collective_id=0, has_side_effects=True, vmem_limit_bytes=66 * 1000 * 1000),
    )(carried, branch_in, up_weight, down_weight, gain_in.reshape(1, dl), bias_in.reshape(1, dl),
      gain_out.reshape(1, dl), bias_out.reshape(1, dl))


def solution(mesh):
    in_specs = (
        P("dp", "ra"),
        P("dp", "ra"),
        P("ra"),
        P("ra"),
        P("ra", "cb"),
        P("cb", "ra"),
        P("ra"),
        P("ra"),
    )
    out_specs = P("dp", "ra")
    return jax.shard_map(
        per_device, mesh=mesh, in_specs=in_specs, out_specs=out_specs, check_vma=False
    )
```
